32 devices in a mesh: fs: 4 (over y, x), tp: 8 (over z, core).
Axes of the slice: x: 2, y: 2, z: 4, core: 2. Of those that a mesh axis runs over, the one named last changes fastest.
Arguments:
- saved_query_latent: bfloat16 [4096, 1536], P('fs', 'tp'), may hold values from -6 to 6
- saved_key_value_latent: bfloat16 [4096, 1024], P('fs', 'tp'), may hold values from -6 to 6
- query_cot: bfloat16 [4096, 6144], P('fs', 'tp'), may hold values from -0.09375 to 0.09375
- kv_cot: bfloat16 [4096, 8192], P('fs', 'tp'), may hold values from -0.09375 to 0.09375
- query_full_weight: float32 [1536, 6144], P('fs', 'tp'), may hold values from -0.6 to 0.6
- key_value_full_weight: float32 [1024, 8192], P('fs', 'tp'), may hold values from -0.6 to 0.6
- query_mom: float32 [1536, 6144], P('fs', 'tp'), may hold values from -50 to 50
- kv_mom: float32 [1024, 8192], P('fs', 'tp'), may hold values from -50 to 50
- query_left: bfloat16 [1536, 1536], P('fs'), may hold values from -1 to 1.5
- kv_left: bfloat16 [1024, 1024], P('fs'), may hold values from -1 to 1.5
- query_right: bfloat16 [32, 192, 192], P('tp'), may hold values from -1 to 1.5
- kv_right: bfloat16 [32, 256, 256], P('tp'), may hold values from -1 to 1.5
Outputs:
- query_mom_new: float32 [1536, 6144], P('fs', 'tp')
- kv_mom_new: float32 [1024, 8192], P('fs', 'tp')
- query_update: float32 [1536, 6144], P('fs', 'tp')
- kv_update: float32 [1024, 8192], P('fs', 'tp')
- query_weight: float32 [1536, 6144], P('fs', 'tp')
- kv_weight: float32 [1024, 8192], P('fs', 'tp')
- query_copy: bfloat16 [1536, 6144], P(None, 'tp')
- kv_copy: bfloat16 [1024, 8192], P(None, 'tp')
The draws below stay inside these ranges and needn't reach their ends.
All inputs are finite; a program needn't handle non-finite values.
Results may differ from the reference program's by a relative error of at most 0.0055.
Values may be sent and summed in bfloat16 or wider, within the bound.
A program may use at most 64 MiB of HBM per device.

```python
import jax
import jax.numpy as jnp

QUERY_RANK = 1536
KEY_VALUE_RANK = 1024
HEAD_COUNT = 32
QUERY_KEY_WIDTH = 192
KEY_VALUE_WIDTH = 256
TOKEN_COUNT = 4096


def increasing_order(key, rows, cols):
    base = jax.random.truncated_normal(key, -5.0, 5.0, (rows, cols), jnp.float32)
    row_scale = 10.0 ** (jnp.arange(rows, dtype=jnp.float32) / max(rows - 1, 1))
    col_scale = 10.0 ** (jnp.arange(cols, dtype=jnp.float32) / max(cols - 1, 1))
    return 0.1 * base * row_scale[:, None] * col_scale[None, :]


def positive_definite(key, order):
    first = jax.random.fold_in(key, 11)
    second = jax.random.fold_in(key, 12)
    off = jax.random.truncated_normal(first, -5.0, 5.0, (order, order), jnp.float32)
    off = (off + off.T) * (0.3 / (2.0 * order) ** 0.5)
    diag = jax.random.uniform(second, (order,), jnp.float32, 0.9, 1.5)
    eye = jnp.eye(order, dtype=jnp.float32)
    return off * (1.0 - eye) + eye * diag[None, :]


def draw_query_mom(key, part):
    return increasing_order(jax.random.fold_in(key, 1), QUERY_RANK, HEAD_COUNT * QUERY_KEY_WIDTH)


def draw_kv_mom(key, part):
    return increasing_order(jax.random.fold_in(key, 2), KEY_VALUE_RANK, HEAD_COUNT * KEY_VALUE_WIDTH)


def draw_query_left(key, part):
    return positive_definite(jax.random.fold_in(key, 3), QUERY_RANK).astype(jnp.bfloat16)


def draw_kv_left(key, part):
    return positive_definite(jax.random.fold_in(key, 4), KEY_VALUE_RANK).astype(jnp.bfloat16)


def draw_query_right(key, part):
    keys = jax.random.split(jax.random.fold_in(key, 5), HEAD_COUNT)
    return jax.vmap(lambda single: positive_definite(single, QUERY_KEY_WIDTH))(keys).astype(jnp.bfloat16)


def draw_kv_right(key, part):
    keys = jax.random.split(jax.random.fold_in(key, 6), HEAD_COUNT)
    return jax.vmap(lambda single: positive_definite(single, KEY_VALUE_WIDTH))(keys).astype(jnp.bfloat16)


def raised(result, key, source, target, blocks, factor):
    owner, partner = [(jnp.arange(result.shape[position]) // (result.shape[position] // blocks)).reshape([-1 if axis == position else 1 for axis in range(result.ndim)]) for position in (source, target)]
    chosen = jax.random.permutation(key, blocks)[partner]
    strong = (owner == chosen) | (owner == (partner + blocks // 2) % blocks)
    return jnp.where(strong, factor * result, result)


def levels(rng, extent, cuts, low, largest):
    def one(position, parts):
        steps = jax.random.uniform(jax.random.fold_in(jax.random.fold_in(rng, 6), position), (parts,), jnp.float32, low / len(cuts), largest / len(cuts))
        return jnp.repeat(jnp.exp(steps), extent[position] // parts).reshape((-1,) + (1,) * (len(extent) - position - 1))

    gain = one(*cuts[0])
    for cut in cuts[1:]:
        gain = gain * one(*cut)
    return gain


def centred(own_key, dims, spread, reach, shards=(), kind=jnp.bfloat16):
    result = spread * jax.random.normal(own_key, dims, jnp.float32)
    if shards:
        result = result * levels(own_key, dims, shards, -0.22, 0.18)
    return jnp.clip(result, -reach, reach).astype(kind)


def noise_with(stream_key, dims, deviation, most, pieces, heavy, kind=jnp.bfloat16):
    result = deviation * jax.random.normal(stream_key, dims, jnp.float32)
    if pieces:
        result = result * levels(stream_key, dims, pieces, -0.22, 0.18)
    return jnp.clip(raised(result, jax.random.fold_in(stream_key, 3), *heavy), -most, most).astype(kind)


def setup_inputs(seed: int = 0) -> dict:
    key_list = jax.random.split(jax.random.key(seed), 13)
    saved_query_latent = noise_with(key_list[0], (TOKEN_COUNT, QUERY_RANK), 1.0, 6.0, ((0, 4), (1, 8)), (0, 1, 8, 2.0))
    saved_key_value_latent = noise_with(key_list[1], (TOKEN_COUNT, KEY_VALUE_RANK), 1.0, 6.0, ((0, 4), (1, 8)), (0, 1, 8, 2.0))
    query_cot = centred(key_list[2], (TOKEN_COUNT, HEAD_COUNT * QUERY_KEY_WIDTH), (1.0 / TOKEN_COUNT ** 0.5), 0.09375, ((0, 4), (1, 8)))
    kv_cot = centred(key_list[3], (TOKEN_COUNT, HEAD_COUNT * KEY_VALUE_WIDTH), (1.0 / TOKEN_COUNT ** 0.5), 0.09375, ((0, 4), (1, 8)))
    query_full_weight = centred(key_list[4], (QUERY_RANK, HEAD_COUNT * QUERY_KEY_WIDTH), 0.1, 0.6, ((0, 4), (1, 8)), jnp.float32)
    key_value_full_weight = centred(key_list[5], (KEY_VALUE_RANK, HEAD_COUNT * KEY_VALUE_WIDTH), 0.1, 0.6, ((0, 4), (1, 8)), jnp.float32)
    query_mom = draw_query_mom(jax.random.fold_in(key_list[12], 71), 0)
    kv_mom = draw_kv_mom(jax.random.fold_in(key_list[12], 71), 0)
    query_left = draw_query_left(jax.random.fold_in(key_list[12], 71), 0)
    kv_left = draw_kv_left(jax.random.fold_in(key_list[12], 71), 0)
    query_right = draw_query_right(jax.random.fold_in(key_list[12], 71), 0)
    kv_right = draw_kv_right(jax.random.fold_in(key_list[12], 71), 0)
    return dict(saved_query_latent=saved_query_latent, saved_key_value_latent=saved_key_value_latent, query_cot=query_cot, kv_cot=kv_cot, query_full_weight=query_full_weight, key_value_full_weight=key_value_full_weight, query_mom=query_mom, kv_mom=kv_mom, query_left=query_left, kv_left=kv_left, query_right=query_right, kv_right=kv_right)


beta_mom = 0.9
learn_rate = 0.01

def precondition(moment, left, right, heads, width):
    half = moment.astype(jnp.bfloat16)
    pre_left = jnp.dot(left, half, preferred_element_type=jnp.float32)
    left_half = pre_left.astype(jnp.bfloat16).astype(jnp.float32)
    blocks = left_half.reshape(left_half.shape[0], heads, width)
    pre = jnp.einsum('rhd,hde->rhe', blocks, right.astype(jnp.float32))
    return pre.reshape(left_half.shape[0], heads * width)

def reference(saved_query_latent, saved_key_value_latent, query_cot, kv_cot, query_full_weight, key_value_full_weight, query_mom, kv_mom, query_left, kv_left, query_right, kv_right):
    query_grad = jnp.dot(saved_query_latent.astype(jnp.float32).T, query_cot.astype(jnp.float32))
    kv_grad = jnp.dot(saved_key_value_latent.astype(jnp.float32).T, kv_cot.astype(jnp.float32))
    query_mom_new = beta_mom * query_mom + query_grad
    kv_mom_new = beta_mom * kv_mom + kv_grad
    query_pre = precondition(query_mom_new, query_left, query_right, HEAD_COUNT, QUERY_KEY_WIDTH)
    kv_pre = precondition(kv_mom_new, kv_left, kv_right, HEAD_COUNT, KEY_VALUE_WIDTH)
    query_scale = jnp.sqrt(jnp.sum(query_mom_new * query_mom_new) / jnp.sum(query_pre * query_pre))
    kv_scale = jnp.sqrt(jnp.sum(kv_mom_new * kv_mom_new) / jnp.sum(kv_pre * kv_pre))
    query_update = query_scale * query_pre
    kv_update = kv_scale * kv_pre
    query_weight = query_full_weight - learn_rate * query_update
    kv_weight = key_value_full_weight - learn_rate * kv_update
    return (query_mom_new, kv_mom_new, query_update, kv_update, query_weight, kv_weight, query_weight.astype(jnp.bfloat16), kv_weight.astype(jnp.bfloat16))
```

```python
import functools

import jax
import jax.numpy as jnp
from jax import lax
from jax.experimental import pallas as pl
from jax.experimental.pallas import tpu as pltpu
from jax.sharding import PartitionSpec as P

MESH = pl.DeviceIdType.MESH
beta_mom = 0.9
learn_rate = 0.01


def col_tile(cols):
    return 256 if cols % 256 == 0 else cols


def rcopy(src, dst, send, recv, dev):
    return pltpu.make_async_remote_copy(
        src_ref=src, dst_ref=dst, send_sem=send, recv_sem=recv, device_id=dev, device_id_type=MESH
    )


def kernel(nf, nt, *refs):
    (lat, cot_h, w_h, mom_h, left_h, right_h) = [refs[2 * i : 2 * i + 2] for i in range(6)]
    outs = refs[12:20]
    mom_o, upd_o, wgt_o, cpy_o = [outs[2 * i : 2 * i + 2] for i in range(4)]
    s = refs[20:]
    cot, w, mom, left, right, lat_all, own, pb, rb, half, pre, cpy, stf, stt, st0, st1 = [
        s[2 * i : 2 * i + 2] for i in range(16)
    ]
    (in_sem, out_sem, bar_a_up, a_dn, a_sib_u, a_sib_d, a_recv, b_send, b_recv, g_send, g_recv,
     sf_send, sf_recv, st_send, st_recv) = s[32:]
    a_up = bar_a_up

    f = lax.axis_index("fs")
    t = lax.axis_index("tp")
    nz = nt // 2
    z = t // 2
    c = t % 2
    sib = z * 2 + (1 - c)

    loads = []
    for m in range(2):
        for i, (src, dst) in enumerate(
            [(cot_h[m], cot[m]), (mom_h[m], mom[m]), (left_h[m], left[m]), (right_h[m], right[m]), (w_h[m], w[m])]
        ):
            cp = pltpu.make_async_copy(src, dst, in_sem.at[m, i])
            cp.start()
            loads.append(cp)
    load = lambda m, i: loads[5 * m + i]

    rt = [lat[m].shape[0] for m in range(2)]
    rows = [2 * r for r in rt]
    cols = [cot[m].shape[1] for m in range(2)]

    def shard(m, k, core):
        return lat_all[m].at[k, pl.ds(pl.multiple_of(core * rt[m], rt[m]), rt[m])]

    local = []
    for m in range(2):
        cp = pltpu.make_async_copy(lat[m], shard(m, z, c), in_sem.at[m, 5])
        cp.start()
        local.append(cp)

    barrier = pltpu.get_barrier_semaphore()
    for d in range(1, nf):
        pl.semaphore_signal(barrier, inc=1, device_id={"fs": (f + d) % nf}, device_id_type=MESH)
    for d in range(1, nt):
        pl.semaphore_signal(barrier, inc=1, device_id={"tp": (t + d) % nt}, device_id_type=MESH)
    pl.semaphore_wait(barrier, nf + nt - 2)

    def up(m, i, k, src=None):
        return rcopy(
            shard(m, k, c) if src is None else src, shard(m, k, c), a_up.at[m, i], a_recv.at[m, k, c], {"tp": t + 2}
        )

    def down(m, i, k, src=None):
        return rcopy(
            shard(m, k, c) if src is None else src, shard(m, k, c), a_dn.at[m, i], a_recv.at[m, k, c], {"tp": t - 2}
        )

    def across(m, sem, k, src=None):
        return rcopy(
            shard(m, k, c) if src is None else src, shard(m, k, c), sem, a_recv.at[m, k, c], {"tp": sib}
        )

    def own_up(m):
        @pl.when(z < nz - 1)
        def _():
            up(m, 0, z, lat[m]).start()

    def own_down(m):
        @pl.when(z > 0)
        def _():
            down(m, 0, z, lat[m]).start()

    def wait_shard(m, k, core):
        x = shard(m, k, core)
        rcopy(x, x, a_up.at[m, 0], a_recv.at[m, k, core], {"tp": sib}).wait_recv()

    def partial(m, k):
        tile = col_tile(cols[m])

        def body(i, carry):
            cs = pl.ds(pl.multiple_of(i * tile, tile), tile)
            p = jnp.dot(lat_all[m][k], cot[m][:, cs], preferred_element_type=jnp.float32)

            @pl.when(k == f)
            def _():
                own[m][:, cs] = p

            @pl.when(k != f)
            def _():
                pb[m][k, :, cs] = p.astype(jnp.bfloat16)

            return carry

        lax.fori_loop(0, cols[m] // tile, body, 0)

        @pl.when(k != f)
        def _():
            rcopy(pb[m].at[k], rb[m].at[f], b_send.at[m, k], b_recv.at[m, f], {"fs": k}).start()

    own_up(0)
    own_down(0)
    for m in range(2):
        across(m, a_sib_u.at[m, 0], z, lat[m]).start()

    for m in range(2):
        if m == 0:
            pl.when(z == 0)(lambda: own_up(1))
            pl.when(z == nz - 1)(lambda: own_down(1))
        load(m, 0).wait()
        local[m].wait()
        wait_shard(m, z, 1 - c)
        partial(m, z)

        def step(i, carry, m=m):
            lo, hi = z - i, z + i

            @pl.when(lo >= 0)
            def _():
                wait_shard(m, lo, c)

                @pl.when(z < nz - 1)
                def _():
                    up(m, i, lo).start()

                across(m, a_sib_u.at[m, i], lo).start()

            @pl.when(hi < nz)
            def _():
                wait_shard(m, hi, c)

                @pl.when(z > 0)
                def _():
                    down(m, i, hi).start()

                across(m, a_sib_d.at[m, i], hi).start()

            if m == 0:
                pl.when(z == i)(lambda: own_up(1))
                pl.when(z == nz - 1 - i)(lambda: own_down(1))

            @pl.when(lo >= 0)
            def _():
                wait_shard(m, lo, 1 - c)
                partial(m, lo)

            @pl.when(hi < nz)
            def _():
                wait_shard(m, hi, 1 - c)
                partial(m, hi)

            return carry

        lax.fori_loop(1, nz, step, 0)

    relay = nf == 4
    xn = (f // 2) * 2 + (1 - f % 2)
    yn = (1 - f // 2) * 2 + f % 2
    dn = 3 - f

    def block(buf, m, g, part=None):
        r = rows[m]
        if part is None:
            return buf[m].at[pl.ds(pl.multiple_of(g * r, r), r)]
        return buf[m].at[pl.ds(pl.multiple_of(g * r + part * (r // 2), r // 2), r // 2)]

    def g_copy(ph, buf, m, i, g, dev, part=None):
        b = block(buf, m, g, part)
        return rcopy(b, b, g_send.at[ph, m, i], g_recv.at[ph, m, i], {"fs": dev})

    def gather_own(ph, buf, m):
        if relay:
            g_copy(ph, buf, m, 0, f, xn).start()
            g_copy(ph, buf, m, 1, f, yn).start()
        else:
            for d in range(1, nf):
                g_copy(ph, buf, m, d, f, (f + d) % nf).start()

    def gather_forward(ph, buf, m):
        if relay:
            g_copy(ph, buf, m, 0, xn, xn).wait_recv()
            g_copy(ph, buf, m, 2, xn, yn, 0).start()
            g_copy(ph, buf, m, 1, yn, yn).wait_recv()
            g_copy(ph, buf, m, 3, yn, xn, 1).start()

    def gather_finish(ph, buf, m):
        if relay:
            g_copy(ph, buf, m, 2, dn, yn, 0).wait_recv()
            g_copy(ph, buf, m, 3, dn, xn, 1).wait_recv()
        else:
            for d in range(1, nf):
                g_copy(ph, buf, m, d, (f + nf - d) % nf, f).wait_recv()

    def gather_drain(ph, buf, m):
        if relay:
            g_copy(ph, buf, m, 0, f, xn).wait_send()
            g_copy(ph, buf, m, 1, f, yn).wait_send()
            g_copy(ph, buf, m, 2, xn, yn, 0).wait_send()
            g_copy(ph, buf, m, 3, yn, xn, 1).wait_send()
        else:
            for d in range(1, nf):
                g_copy(ph, buf, m, d, f, (f + d) % nf).wait_send()

    def reduce_momentum(m):
        load(m, 1).wait()
        for d in range(1, nf):
            g = (f + d) % nf
            rcopy(rb[m].at[g], rb[m].at[g], b_send.at[m, 0], b_recv.at[m, g], {"fs": g}).wait_recv()
        tile = col_tile(cols[m])
        r = rows[m]

        def body(i, acc):
            cs = pl.ds(pl.multiple_of(i * tile, tile), tile)
            g = own[m][:, cs]
            for d in range(1, nf):
                g = g + rb[m][(f + d) % nf, :, cs].astype(jnp.float32)
            new = beta_mom * mom[m][:, cs] + g
            mom[m][:, cs] = new
            half[m][pl.ds(pl.multiple_of(f * r, r), r), cs] = new.astype(jnp.bfloat16)
            return acc + jnp.sum(new * new, axis=0, keepdims=True)

        acc = lax.fori_loop(0, cols[m] // tile, body, jnp.zeros((1, tile), jnp.float32))
        gather_own(0, half, m)
        pltpu.make_async_copy(mom[m], mom_o[m], out_sem.at[m, 0]).start()
        return jnp.sum(acc)

    def direction(m, msq):
        load(m, 2).wait()
        load(m, 3).wait()
        width = right[m].shape[1]

        def body(i, acc):
            cs = pl.ds(pl.multiple_of(i * width, width), width)
            lh = jnp.dot(left[m][...], half[m][:, cs], preferred_element_type=jnp.float32)
            p = jnp.dot(lh.astype(jnp.bfloat16), right[m][i], preferred_element_type=jnp.float32)
            pre[m][:, cs] = p
            return acc + jnp.sum(p * p, axis=0, keepdims=True)

        acc = lax.fori_loop(0, cols[m] // width, body, jnp.zeros((1, width), jnp.float32))
        st0[m][0:8, :] = jnp.full((8, 128), msq, jnp.float32)
        st0[m][8:16, :] = jnp.full((8, 128), jnp.sum(acc), jnp.float32)
        for d in range(1, nt):
            rcopy(st0[m], stt[m].at[d], st_send.at[m, d], st_recv.at[m, d], {"tp": (t + d) % nt}).start()

    def stats_tp(m):
        tot = st0[m][...]
        for d in range(1, nt):
            rcopy(st0[m], stt[m].at[d], st_send.at[m, d], st_recv.at[m, d], {"tp": sib}).wait_recv()
            tot = tot + stt[m][d]
        st1[m][...] = tot
        for d in range(1, nf):
            rcopy(st1[m], stf[m].at[d], sf_send.at[m, d], sf_recv.at[m, d], {"fs": (f + d) % nf}).start()

    def finish(m):
        tot = st1[m][...]
        for d in range(1, nf):
            rcopy(st1[m], stf[m].at[d], sf_send.at[m, d], sf_recv.at[m, d], {"fs": f}).wait_recv()
            tot = tot + stf[m][d]
        scale = jnp.sqrt(tot[0:1, 0:1] / tot[8:9, 0:1])
        load(m, 4).wait()
        tile = col_tile(cols[m])
        r = rows[m]

        def body(i, carry):
            cs = pl.ds(pl.multiple_of(i * tile, tile), tile)
            u = scale * pre[m][:, cs]
            new = w[m][:, cs] - learn_rate * u
            pre[m][:, cs] = u
            w[m][:, cs] = new
            cpy[m][pl.ds(pl.multiple_of(f * r, r), r), cs] = new.astype(jnp.bfloat16)
            return carry

        lax.fori_loop(0, cols[m] // tile, body, 0)
        gather_own(1, cpy, m)
        pltpu.make_async_copy(pre[m], upd_o[m], out_sem.at[m, 1]).start()
        pltpu.make_async_copy(w[m], wgt_o[m], out_sem.at[m, 2]).start()

    msq0 = reduce_momentum(0)
    msq1 = reduce_momentum(1)
    gather_forward(0, half, 0)
    gather_finish(0, half, 0)
    direction(0, msq0)
    gather_forward(0, half, 1)
    stats_tp(0)
    finish(0)
    gather_finish(0, half, 1)
    direction(1, msq1)
    stats_tp(1)
    gather_forward(1, cpy, 0)
    finish(1)
    gather_finish(1, cpy, 0)
    pltpu.make_async_copy(cpy[0], cpy_o[0], out_sem.at[0, 3]).start()
    gather_forward(1, cpy, 1)
    gather_finish(1, cpy, 1)
    pltpu.make_async_copy(cpy[1], cpy_o[1], out_sem.at[1, 3]).start()

    for m in range(2):
        gather_drain(0, half, m)
        gather_drain(1, cpy, m)
        for d in range(1, nt):
            rcopy(st0[m], stt[m].at[d], st_send.at[m, d], st_recv.at[m, d], {"tp": (t + d) % nt}).wait_send()
        for d in range(1, nf):
            rcopy(st1[m], stf[m].at[d], sf_send.at[m, d], sf_recv.at[m, d], {"fs": (f + d) % nf}).wait_send()
            g = (f + d) % nf
            rcopy(pb[m].at[g], rb[m].at[f], b_send.at[m, g], b_recv.at[m, f], {"fs": g}).wait_send()

        across(m, a_sib_u.at[m, 0], z).wait_send()

        def drain(i, carry, m=m):
            lo, hi = z - i, z + i

            @pl.when((lo >= 0) & (z < nz - 1))
            def _():
                up(m, i, lo).wait_send()

            @pl.when((hi < nz) & (z > 0))
            def _():
                down(m, i, hi).wait_send()

            @pl.when((lo >= 0) & (i > 0))
            def _():
                across(m, a_sib_u.at[m, i], lo).wait_send()

            @pl.when((hi < nz) & (i > 0))
            def _():
                across(m, a_sib_d.at[m, i], hi).wait_send()

            return carry

        lax.fori_loop(0, nz, drain, 0)
        for i, (src, dst) in enumerate([(mom[m], mom_o[m]), (pre[m], upd_o[m]), (w[m], wgt_o[m]), (cpy[m], cpy_o[m])]):
            pltpu.make_async_copy(src, dst, out_sem.at[m, i]).wait()


def paired(right):
    heads, width = right.shape[0], right.shape[1]
    if width % 128 == 0 or heads % 2:
        return right
    a, b = right[0::2], right[1::2]
    zero = jnp.zeros_like(a)
    return jnp.concatenate(
        [jnp.concatenate([a, zero], axis=2), jnp.concatenate([zero, b], axis=2)], axis=1
    )


def on_device(nf, nt, q_lat, kv_lat, q_cot, kv_cot, q_w, kv_w, q_mom, kv_mom, q_left, kv_left, q_right, kv_right):
    lats = (kv_lat.T, q_lat.T)
    cots, ws, moms, lefts = (kv_cot, q_cot), (kv_w, q_w), (kv_mom, q_mom), (kv_left, q_left)
    rights = (paired(kv_right), paired(q_right))
    bf, f32 = jnp.bfloat16, jnp.float32
    sds = jax.ShapeDtypeStruct
    f32_out = [sds(x.shape, f32) for x in ws]
    cpy_out = [sds((x.shape[0] * nf, x.shape[1]), bf) for x in ws]
    V = pltpu.VMEM
    nz = nt // 2

    def both(make):
        return [make(m) for m in range(2)]

    scratch = (
        both(lambda m: V(cots[m].shape, bf))
        + both(lambda m: V(ws[m].shape, f32))
        + both(lambda m: V(moms[m].shape, f32))
        + both(lambda m: V(lefts[m].shape, bf))
        + both(lambda m: V(rights[m].shape, bf))
        + both(lambda m: V((nz, 2 * lats[m].shape[0], lats[m].shape[1]), bf))
        + both(lambda m: V(ws[m].shape, f32))
        + both(lambda m: V((nf,) + ws[m].shape, bf))
        + both(lambda m: V((nf,) + ws[m].shape, bf))
        + both(lambda m: V(cpy_out[m].shape, bf))
        + both(lambda m: V(ws[m].shape, f32))
        + both(lambda m: V(cpy_out[m].shape, bf))
        + both(lambda m: V((nf, 16, 128), f32))
        + both(lambda m: V((nt, 16, 128), f32))
        + both(lambda m: V((16, 128), f32))
        + both(lambda m: V((16, 128), f32))
    )
    D = pltpu.SemaphoreType.DMA
    ng = max(nf, 4)
    sems = [
        D((2, 6)), D((2, 4)), D((2, nz)), D((2, nz)), D((2, nz)), D((2, nz)), D((2, nz, 2)),
        D((2, nf)), D((2, nf)), D((2, 2, ng)), D((2, 2, ng)),
        D((2, nf)), D((2, nf)), D((2, nt)), D((2, nt)),
    ]
    any_spec = pl.BlockSpec(memory_space=pl.ANY)
    vmem_spec = pl.BlockSpec(memory_space=pltpu.VMEM)
    out = pl.pallas_call(
        functools.partial(kernel, nf, nt),
        out_shape=f32_out + f32_out + f32_out + cpy_out,
        in_specs=[vmem_spec] * 2 + [any_spec] * 10,
        out_specs=[any_spec] * 8,
        scratch_shapes=scratch + sems,
        compiler_params=pltpu.CompilerParams(
            collective_id=0, has_side_effects=True, vmem_limit_bytes=60 * 1024 * 1024
        ),
    )(*lats, *cots, *ws, *moms, *lefts, *rights)
    return (out[1], out[0], out[3], out[2], out[5], out[4], out[7], out[6])


def solution(mesh):
    nf, nt = mesh.shape["fs"], mesh.shape["tp"]
    placed = (P("fs", "tp"),) * 8 + (P("fs", None),) * 2 + (P("tp", None, None),) * 2
    return jax.shard_map(
        functools.partial(on_device, nf, nt),
        mesh=mesh,
        in_specs=placed,
        out_specs=(P("fs", "tp"),) * 6 + (P(None, "tp"),) * 2,
        check_vma=False,
    )
```

```python
import functools

import jax
import jax.numpy as jnp
from jax import lax
from jax.experimental import pallas as pl
from jax.experimental.pallas import tpu as pltpu
from jax.sharding import PartitionSpec as P

MESH = pl.DeviceIdType.MESH
beta_mom = 0.9
learn_rate = 0.01


def col_tile(cols):
    return 256 if cols % 256 == 0 else cols


def rcopy(src, dst, send, recv, dev):
    return pltpu.make_async_remote_copy(
        src_ref=src, dst_ref=dst, send_sem=send, recv_sem=recv, device_id=dev, device_id_type=MESH
    )


def kernel(nf, nt, *refs):
    (lat, cot_h, w_h, mom_h, left_h, right_h) = [refs[2 * i : 2 * i + 2] for i in range(6)]
    outs = refs[12:20]
    mom_o, upd_o, wgt_o, cpy_o = [outs[2 * i : 2 * i + 2] for i in range(4)]
    s = refs[20:]
    cot, w, mom, left, right, lat_all, own, pb, rb, half, pre, cpy, stf, stt, st0, st1 = [
        s[2 * i : 2 * i + 2] for i in range(16)
    ]
    (in_sem, out_sem, bar_a_up, a_dn, a_sib_u, a_sib_d, a_recv, b_send, b_recv, g_send, g_recv,
     sf_send, sf_recv, st_send, st_recv) = s[32:]
    a_up = bar_a_up

    f = lax.axis_index("fs")
    t = lax.axis_index("tp")
    nz = nt // 2
    z = t // 2
    c = t % 2
    sib = z * 2 + (1 - c)

    loads = []
    for m in range(2):
        for i, (src, dst) in enumerate(
            [(cot_h[m], cot[m]), (mom_h[m], mom[m]), (left_h[m], left[m]), (right_h[m], right[m]), (w_h[m], w[m])]
        ):
            cp = pltpu.make_async_copy(src, dst, in_sem.at[m, i])
            cp.start()
            loads.append(cp)
    load = lambda m, i: loads[5 * m + i]

    rt = [lat[m].shape[0] for m in range(2)]
    rows = [2 * r for r in rt]
    cols = [cot[m].shape[1] for m in range(2)]

    def shard(m, k, core):
        return lat_all[m].at[k, pl.ds(pl.multiple_of(core * rt[m], rt[m]), rt[m])]

    local = []
    for m in range(2):
        cp = pltpu.make_async_copy(lat[m], shard(m, z, c), in_sem.at[m, 5])
        cp.start()
        local.append(cp)

    barrier = pltpu.get_barrier_semaphore()
    for d in range(1, nf):
        pl.semaphore_signal(barrier, inc=1, device_id={"fs": (f + d) % nf}, device_id_type=MESH)
    for d in range(1, nt):
        pl.semaphore_signal(barrier, inc=1, device_id={"tp": (t + d) % nt}, device_id_type=MESH)
    pl.semaphore_wait(barrier, nf + nt - 2)

    def up(m, i, k, src=None):
        return rcopy(
            shard(m, k, c) if src is None else src, shard(m, k, c), a_up.at[m, i], a_recv.at[m, k, c], {"tp": t + 2}
        )

    def down(m, i, k, src=None):
        return rcopy(
            shard(m, k, c) if src is None else src, shard(m, k, c), a_dn.at[m, i], a_recv.at[m, k, c], {"tp": t - 2}
        )

    def across(m, sem, k, src=None):
        return rcopy(
            shard(m, k, c) if src is None else src, shard(m, k, c), sem, a_recv.at[m, k, c], {"tp": sib}
        )

    def own_up(m):
        @pl.when(z < nz - 1)
        def _():
            up(m, 0, z, lat[m]).start()

    def own_down(m):
        @pl.when(z > 0)
        def _():
            down(m, 0, z, lat[m]).start()

    def wait_shard(m, k, core):
        x = shard(m, k, core)
        rcopy(x, x, a_up.at[m, 0], a_recv.at[m, k, core], {"tp": sib}).wait_recv()

    def partial(m, k):
        tile = col_tile(cols[m])

        def body(i, carry):
            cs = pl.ds(pl.multiple_of(i * tile, tile), tile)
            p = jnp.dot(lat_all[m][k], cot[m][:, cs], preferred_element_type=jnp.float32)

            @pl.when(k == f)
            def _():
                own[m][:, cs] = p

            @pl.when(k != f)
            def _():
                pb[m][k, :, cs] = p.astype(jnp.bfloat16)

            return carry

        lax.fori_loop(0, cols[m] // tile, body, 0)

        @pl.when(k != f)
        def _():
            rcopy(pb[m].at[k], rb[m].at[f], b_send.at[m, k], b_recv.at[m, f], {"fs": k}).start()

    own_up(0)
    own_down(0)
    for m in range(2):
        across(m, a_sib_u.at[m, 0], z, lat[m]).start()

    for m in range(2):
        if m == 0:
            pl.when(z == 0)(lambda: own_up(1))
            pl.when(z == nz - 1)(lambda: own_down(1))
        load(m, 0).wait()
        local[m].wait()
        wait_shard(m, z, 1 - c)
        partial(m, z)

        def step(i, carry, m=m):
            lo, hi = z - i, z + i

            @pl.when(lo >= 0)
            def _():
                wait_shard(m, lo, c)

                @pl.when(z < nz - 1)
                def _():
                    up(m, i, lo).start()

                across(m, a_sib_u.at[m, i], lo).start()

            @pl.when(hi < nz)
            def _():
                wait_shard(m, hi, c)

                @pl.when(z > 0)
                def _():
                    down(m, i, hi).start()

                across(m, a_sib_d.at[m, i], hi).start()

            if m == 0:
                pl.when(z == i)(lambda: own_up(1))
                pl.when(z == nz - 1 - i)(lambda: own_down(1))

            @pl.when(lo >= 0)
            def _():
                wait_shard(m, lo, 1 - c)
                partial(m, lo)

            @pl.when(hi < nz)
            def _():
                wait_shard(m, hi, 1 - c)
                partial(m, hi)

            return carry

        lax.fori_loop(1, nz, step, 0)

    relay = nf == 4
    xn = (f // 2) * 2 + (1 - f % 2)
    yn = (1 - f // 2) * 2 + f % 2
    dn = 3 - f

    def block(buf, m, g, part=None):
        r = rows[m]
        if part is None:
            return buf[m].at[pl.ds(pl.multiple_of(g * r, r), r)]
        return buf[m].at[pl.ds(pl.multiple_of(g * r + part * (r // 2), r // 2), r // 2)]

    def g_copy(ph, buf, m, i, g, dev, part=None):
        b = block(buf, m, g, part)
        return rcopy(b, b, g_send.at[ph, m, i], g_recv.at[ph, m, i], {"fs": dev})

    def gather_own(ph, buf, m):
        if relay:
            g_copy(ph, buf, m, 0, f, xn).start()
            g_copy(ph, buf, m, 1, f, yn).start()
        else:
            for d in range(1, nf):
                g_copy(ph, buf, m, d, f, (f + d) % nf).start()

    def gather_forward(ph, buf, m):
        if relay:
            g_copy(ph, buf, m, 0, xn, xn).wait_recv()
            g_copy(ph, buf, m, 2, xn, yn, 0).start()
            g_copy(ph, buf, m, 1, yn, yn).wait_recv()
            g_copy(ph, buf, m, 3, yn, xn, 1).start()

    def gather_finish(ph, buf, m):
        if relay:
            g_copy(ph, buf, m, 2, dn, yn, 0).wait_recv()
            g_copy(ph, buf, m, 3, dn, xn, 1).wait_recv()
        else:
            for d in range(1, nf):
                g_copy(ph, buf, m, d, (f + nf - d) % nf, f).wait_recv()

    def gather_drain(ph, buf, m):
        if relay:
            g_copy(ph, buf, m, 0, f, xn).wait_send()
            g_copy(ph, buf, m, 1, f, yn).wait_send()
            g_copy(ph, buf, m, 2, xn, yn, 0).wait_send()
            g_copy(ph, buf, m, 3, yn, xn, 1).wait_send()
        else:
            for d in range(1, nf):
                g_copy(ph, buf, m, d, f, (f + d) % nf).wait_send()

    def reduce_momentum(m):
        load(m, 1).wait()
        for d in range(1, nf):
            g = (f + d) % nf
            rcopy(rb[m].at[g], rb[m].at[g], b_send.at[m, 0], b_recv.at[m, g], {"fs": g}).wait_recv()
        tile = col_tile(cols[m])
        r = rows[m]

        def body(i, acc):
            cs = pl.ds(pl.multiple_of(i * tile, tile), tile)
            g = own[m][:, cs]
            for d in range(1, nf):
                g = g + rb[m][(f + d) % nf, :, cs].astype(jnp.float32)
            new = beta_mom * mom[m][:, cs] + g
            mom[m][:, cs] = new
            half[m][pl.ds(pl.multiple_of(f * r, r), r), cs] = new.astype(jnp.bfloat16)
            return acc + jnp.sum(new * new, axis=0, keepdims=True)

        acc = lax.fori_loop(0, cols[m] // tile, body, jnp.zeros((1, tile), jnp.float32))
        gather_own(0, half, m)
        pltpu.make_async_copy(mom[m], mom_o[m], out_sem.at[m, 0]).start()
        return jnp.sum(acc)

    def direction(m, msq):
        load(m, 2).wait()
        load(m, 3).wait()
        head = right[m].shape[1]
        pair = 2 if head % 128 and right[m].shape[0] % 2 == 0 else 1
        width = pair * head

        def body(i, acc):
            cs = pl.ds(pl.multiple_of(i * width, width), width)
            lh = jnp.dot(left[m][...], half[m][:, cs], preferred_element_type=jnp.float32)
            lh = lh.astype(jnp.bfloat16)
            p = jnp.concatenate(
                [
                    jnp.dot(lh[:, j * head : (j + 1) * head], right[m][pair * i + j], preferred_element_type=jnp.float32)
                    for j in range(pair)
                ],
                axis=1,
            )
            pre[m][:, cs] = p
            return acc + jnp.sum(p * p, axis=0, keepdims=True)

        acc = lax.fori_loop(0, cols[m] // width, body, jnp.zeros((1, width), jnp.float32))
        st0[m][0:8, :] = jnp.full((8, 128), msq, jnp.float32)
        st0[m][8:16, :] = jnp.full((8, 128), jnp.sum(acc), jnp.float32)
        for d in range(1, nt):
            rcopy(st0[m], stt[m].at[d], st_send.at[m, d], st_recv.at[m, d], {"tp": (t + d) % nt}).start()

    def stats_tp(m):
        tot = st0[m][...]
        for d in range(1, nt):
            rcopy(st0[m], stt[m].at[d], st_send.at[m, d], st_recv.at[m, d], {"tp": sib}).wait_recv()
            tot = tot + stt[m][d]
        st1[m][...] = tot
        for d in range(1, nf):
            rcopy(st1[m], stf[m].at[d], sf_send.at[m, d], sf_recv.at[m, d], {"fs": (f + d) % nf}).start()

    def finish(m):
        tot = st1[m][...]
        for d in range(1, nf):
            rcopy(st1[m], stf[m].at[d], sf_send.at[m, d], sf_recv.at[m, d], {"fs": f}).wait_recv()
            tot = tot + stf[m][d]
        scale = jnp.sqrt(tot[0:1, 0:1] / tot[8:9, 0:1])
        load(m, 4).wait()
        tile = col_tile(cols[m])
        r = rows[m]

        def body(i, carry):
            cs = pl.ds(pl.multiple_of(i * tile, tile), tile)
            u = scale * pre[m][:, cs]
            new = w[m][:, cs] - learn_rate * u
            pre[m][:, cs] = u
            w[m][:, cs] = new
            cpy[m][pl.ds(pl.multiple_of(f * r, r), r), cs] = new.astype(jnp.bfloat16)
            return carry

        lax.fori_loop(0, cols[m] // tile, body, 0)
        gather_own(1, cpy, m)
        pltpu.make_async_copy(pre[m], upd_o[m], out_sem.at[m, 1]).start()
        pltpu.make_async_copy(w[m], wgt_o[m], out_sem.at[m, 2]).start()

    msq0 = reduce_momentum(0)
    msq1 = reduce_momentum(1)
    gather_forward(0, half, 0)
    gather_finish(0, half, 0)
    direction(0, msq0)
    gather_forward(0, half, 1)
    stats_tp(0)
    finish(0)
    gather_finish(0, half, 1)
    direction(1, msq1)
    stats_tp(1)
    gather_forward(1, cpy, 0)
    finish(1)
    gather_finish(1, cpy, 0)
    pltpu.make_async_copy(cpy[0], cpy_o[0], out_sem.at[0, 3]).start()
    gather_forward(1, cpy, 1)
    gather_finish(1, cpy, 1)
    pltpu.make_async_copy(cpy[1], cpy_o[1], out_sem.at[1, 3]).start()

    for m in range(2):
        gather_drain(0, half, m)
        gather_drain(1, cpy, m)
        for d in range(1, nt):
            rcopy(st0[m], stt[m].at[d], st_send.at[m, d], st_recv.at[m, d], {"tp": (t + d) % nt}).wait_send()
        for d in range(1, nf):
            rcopy(st1[m], stf[m].at[d], sf_send.at[m, d], sf_recv.at[m, d], {"fs": (f + d) % nf}).wait_send()
            g = (f + d) % nf
            rcopy(pb[m].at[g], rb[m].at[f], b_send.at[m, g], b_recv.at[m, f], {"fs": g}).wait_send()

        across(m, a_sib_u.at[m, 0], z).wait_send()

        def drain(i, carry, m=m):
            lo, hi = z - i, z + i

            @pl.when((lo >= 0) & (z < nz - 1))
            def _():
                up(m, i, lo).wait_send()

            @pl.when((hi < nz) & (z > 0))
            def _():
                down(m, i, hi).wait_send()

            @pl.when((lo >= 0) & (i > 0))
            def _():
                across(m, a_sib_u.at[m, i], lo).wait_send()

            @pl.when((hi < nz) & (i > 0))
            def _():
                across(m, a_sib_d.at[m, i], hi).wait_send()

            return carry

        lax.fori_loop(0, nz, drain, 0)
        for i, (src, dst) in enumerate([(mom[m], mom_o[m]), (pre[m], upd_o[m]), (w[m], wgt_o[m]), (cpy[m], cpy_o[m])]):
            pltpu.make_async_copy(src, dst, out_sem.at[m, i]).wait()


def on_device(nf, nt, q_lat, kv_lat, q_cot, kv_cot, q_w, kv_w, q_mom, kv_mom, q_left, kv_left, q_right, kv_right):
    lats = (kv_lat.T, q_lat.T)
    cots, ws, moms, lefts = (kv_cot, q_cot), (kv_w, q_w), (kv_mom, q_mom), (kv_left, q_left)
    rights = (kv_right, q_right)
    bf, f32 = jnp.bfloat16, jnp.float32
    sds = jax.ShapeDtypeStruct
    f32_out = [sds(x.shape, f32) for x in ws]
    cpy_out = [sds((x.shape[0] * nf, x.shape[1]), bf) for x in ws]
    V = pltpu.VMEM
    nz = nt // 2

    def both(make):
        return [make(m) for m in range(2)]

    scratch = (
        both(lambda m: V(cots[m].shape, bf))
        + both(lambda m: V(ws[m].shape, f32))
        + both(lambda m: V(moms[m].shape, f32))
        + both(lambda m: V(lefts[m].shape, bf))
        + both(lambda m: V(rights[m].shape, bf))
        + both(lambda m: V((nz, 2 * lats[m].shape[0], lats[m].shape[1]), bf))
        + both(lambda m: V(ws[m].shape, f32))
        + both(lambda m: V((nf,) + ws[m].shape, bf))
        + both(lambda m: V((nf,) + ws[m].shape, bf))
        + both(lambda m: V(cpy_out[m].shape, bf))
        + both(lambda m: V(ws[m].shape, f32))
        + both(lambda m: V(cpy_out[m].shape, bf))
        + both(lambda m: V((nf, 16, 128), f32))
        + both(lambda m: V((nt, 16, 128), f32))
        + both(lambda m: V((16, 128), f32))
        + both(lambda m: V((16, 128), f32))
    )
    D = pltpu.SemaphoreType.DMA
    ng = max(nf, 4)
    sems = [
        D((2, 6)), D((2, 4)), D((2, nz)), D((2, nz)), D((2, nz)), D((2, nz)), D((2, nz, 2)),
        D((2, nf)), D((2, nf)), D((2, 2, ng)), D((2, 2, ng)),
        D((2, nf)), D((2, nf)), D((2, nt)), D((2, nt)),
    ]
    any_spec = pl.BlockSpec(memory_space=pl.ANY)
    vmem_spec = pl.BlockSpec(memory_space=pltpu.VMEM)
    out = pl.pallas_call(
        functools.partial(kernel, nf, nt),
        out_shape=f32_out + f32_out + f32_out + cpy_out,
        in_specs=[vmem_spec] * 2 + [any_spec] * 10,
        out_specs=[any_spec] * 8,
        scratch_shapes=scratch + sems,
        compiler_params=pltpu.CompilerParams(
            collective_id=0, has_side_effects=True, vmem_limit_bytes=60 * 1024 * 1024
        ),
    )(*lats, *cots, *ws, *moms, *lefts, *rights)
    return (out[1], out[0], out[3], out[2], out[5], out[4], out[7], out[6])


def solution(mesh):
    nf, nt = mesh.shape["fs"], mesh.shape["tp"]
    placed = (P("fs", "tp"),) * 8 + (P("fs", None),) * 2 + (P("tp", None, None),) * 2
    return jax.shard_map(
        functools.partial(on_device, nf, nt),
        mesh=mesh,
        in_specs=placed,
        out_specs=(P("fs", "tp"),) * 6 + (P(None, "tp"),) * 2,
        check_vma=False,
    )
```
